32 devices in a mesh: grp: 2 (over y), sp: 4 (over z), tp: 4 (over x, core).
Axes of the slice: x: 2, y: 2, z: 4, core: 2. Of those that a mesh axis runs over, the one named last changes fastest.
Arguments:
- prompt_rows: bfloat16 [6144, 2048], P(('grp', 'sp')), parts along dimension 0, may hold values from -6 to 6
- norm_gain: float32 [2048], replicated, may hold values from 0.1 to 1.9
- key_weight: bfloat16 [2048, 1024], P(None, 'tp'), may hold values from -0.125 to 0.125
- value_weight: bfloat16 [2048, 1024], P(None, 'tp'), may hold values from -0.125 to 0.125
- new_query: bfloat16 [2048], P(('grp', 'tp')), parts along dimension 0, may hold values from -6 to 6
- score_offset: float32 [16], P('tp'), may hold values from -11.5 to -4
- output_gain: float32 [1024], P('tp'), may hold values from 0.1 to 1.9
Outputs:
- key_cache: bfloat16 [8, 4, 4, 768, 64], P(('grp', 'tp'), 'sp'), parts along dimension 0
- value_cache: bfloat16 [8, 4, 4, 768, 64], P(('grp', 'tp'), 'sp'), parts along dimension 0
- first_read: bfloat16 [2048], P(('grp', 'tp')), parts along dimension 0
The draws below stay inside these ranges and needn't reach their ends.
There are 2 independent parts, one for each index of `grp`. The reference program is written for one: setup_inputs(seed, part) draws one part's arguments, and reference() takes and returns one part's arrays. A program takes and returns all parts, laid end to end along the dimension named above; an argument that names none is the same for every part. Nothing has to cross between parts.
All inputs are finite; a program needn't handle non-finite values.
Results may differ from the reference program's by a relative error of at most 0.0059.
Values may be sent and summed in bfloat16 or wider, within the bound.
A program may use at most 64 MiB of HBM per device.

```python
import jax
import jax.numpy as jnp
from jax import lax

WIDTH = 2048
HEADS = 16
HEAD_DIM = 64
LEN = 3072
HEADS_DEV = 4
SUBS = 1
ROWS = 768
N_SP = 4
N_TP = 4


def steps_of(stream_key, extent, cuts, least, top_value):
    gain, own = 1.0, jax.random.fold_in(stream_key, 6)
    for position, parts in cuts:
        heights = jnp.exp(jax.random.uniform(jax.random.fold_in(own, position), (parts,), jnp.float32, least / len(cuts), top_value / len(cuts)))
        gain = gain * jnp.repeat(heights, extent[position] // parts).reshape([-1 if axis == position else 1 for axis in range(len(extent))])
    return gain


def normal_values(key, extent, scale, most, cuts=(), dtype=jnp.bfloat16):
    level = steps_of(key, extent, cuts, -0.22, 0.18) if cuts else 1.0
    values = jax.random.normal(key, extent, jnp.float32) * scale * level
    return jnp.minimum(jnp.maximum(values, -most), most).astype(dtype)


def setup_inputs(seed: int = 0, part: int = 0) -> dict:
    key_of = jax.random.split(jax.random.key(seed), 8)
    part_splits = jax.random.split(jax.random.fold_in(key_of[7], part), 8)
    return {
        "prompt_rows": normal_values(part_splits[0], (LEN, WIDTH), 1.0, 6.0, ((0, 4),)),
        "norm_gain": jnp.clip(1.0 + 0.18 * jax.random.normal(key_of[1], (WIDTH,), jnp.float32), 0.1, 1.9),
        "key_weight": normal_values(key_of[2], (WIDTH, HEADS * HEAD_DIM), WIDTH ** -0.5, 0.125, ((1, 4),)),
        "value_weight": normal_values(key_of[3], (WIDTH, HEADS * HEAD_DIM), WIDTH ** -0.5, 0.125, ((1, 4),)),
        "new_query": normal_values(part_splits[4], (HEADS * HEAD_DIM,), 1.0, 6.0, ((0, 4),)),
        "score_offset": jnp.clip(-11.5 + 7.5 * jax.random.uniform(key_of[5], (HEADS,), jnp.float32) ** steps_of(key_of[5], (HEADS,), ((0, 4),), -0.2, 0.2), -11.5, -4.0),
        "output_gain": jnp.clip(1.0 + 0.18 * jax.random.normal(key_of[6], (HEADS * HEAD_DIM,), jnp.float32), 0.1, 1.9),
    }


EPSILON = 1e-06

def layout(cache):
    split = cache.reshape(N_SP, SUBS, ROWS, N_TP, HEADS_DEV, HEAD_DIM)
    moved = jnp.transpose(split, (3, 4, 1, 0, 2, 5))
    return moved.reshape(N_TP, N_SP, N_SP, ROWS, HEAD_DIM)

def reference(prompt_rows, norm_gain, key_weight, value_weight, new_query, score_offset, output_gain):
    rows32 = prompt_rows.astype(jnp.float32)
    mean_square = lax.optimization_barrier(jnp.mean(rows32 * rows32, axis=-1, keepdims=True))
    normed = (rows32 * lax.rsqrt(mean_square + EPSILON) * norm_gain).astype(jnp.bfloat16)
    keys = jnp.dot(normed, key_weight, preferred_element_type=jnp.float32).astype(jnp.bfloat16)
    values = jnp.dot(normed, value_weight, preferred_element_type=jnp.float32).astype(jnp.bfloat16)
    keys3 = keys.reshape(LEN, HEADS, HEAD_DIM).astype(jnp.float32)
    values3 = values.reshape(LEN, HEADS, HEAD_DIM).astype(jnp.float32)
    query2 = new_query.reshape(HEADS, HEAD_DIM).astype(jnp.float32)
    scores = jnp.einsum('hd,shd->hs', query2, keys3) * HEAD_DIM ** (-0.5) + score_offset[:, None]
    remain = jax.nn.log_sigmoid(-scores)
    after_sum = lax.cumsum(remain, axis=1, reverse=True) - remain
    sticks = jnp.exp(jax.nn.log_sigmoid(scores) + after_sum).astype(jnp.bfloat16)
    sticks32 = lax.optimization_barrier(sticks).astype(jnp.float32)
    mixed = jnp.einsum('hs,shd->hd', sticks32, values3)
    spread = lax.optimization_barrier(jnp.mean(mixed * mixed, axis=-1, keepdims=True))
    result = mixed * lax.rsqrt(spread + EPSILON) * output_gain.reshape(HEADS, HEAD_DIM)
    return (layout(keys), layout(values), result.reshape(HEADS * HEAD_DIM).astype(jnp.bfloat16))
```

```python
import functools

import jax
import jax.numpy as jnp
from jax import lax
from jax.experimental import pallas as pl
from jax.experimental.pallas import tpu as pltpu
from jax.sharding import PartitionSpec as P

EPSILON = 1e-06


def prefix(value, axis, combine, identity):
    peers, position = (lax.axis_size(axis), lax.axis_index(axis))
    everything = lax.all_gather(value, axis)
    start = jnp.broadcast_to(jnp.asarray(identity, value.dtype), value.shape)

    def hop(k, before):
        at = peers - 1 - k
        reached = at > position
        new = combine(before, everything[at])
        return jnp.where(reached, new, before)

    return lax.fori_loop(0, peers, hop, start)


def normalize(rows, norm_gain):
    rows32 = rows.astype(jnp.float32)
    mean_square = jnp.mean(rows32 * rows32, axis=-1, keepdims=True)
    return (rows32 * lax.rsqrt(mean_square + EPSILON) * norm_gain).astype(jnp.bfloat16)


def project_rows(rows, norm_gain, key_weight, value_weight):
    normed = normalize(rows, norm_gain)
    keys = jnp.dot(normed, key_weight, preferred_element_type=jnp.float32).astype(jnp.bfloat16)
    values = jnp.dot(normed, value_weight, preferred_element_type=jnp.float32).astype(jnp.bfloat16)
    return (keys, values)


def cache_layout(keys, values, head_count):
    devices = lax.axis_size("sp")
    subs = devices // head_count
    depth = keys.shape[1] // head_count
    rows = keys.shape[0] // subs

    def arrange(cache):
        split = cache.reshape(subs, rows, head_count, depth)
        return jnp.transpose(split, (2, 0, 1, 3)).reshape(devices, 1, rows, depth)

    moved_keys, moved_values = (
        lax.all_to_all(arrange(keys), "sp", split_axis=0, concat_axis=1, tiled=True),
        lax.all_to_all(arrange(values), "sp", split_axis=0, concat_axis=1, tiled=True),
    )
    target = (1, 1, devices, rows, depth)
    return (moved_keys.reshape(target), moved_values.reshape(target))


def add_terms(first_part, second_part):
    return first_part + second_part


def read_early(new_query, keys, values, score_offset):
    head_count = score_offset.shape[0]
    depth = keys.shape[1] // head_count
    query2 = new_query.reshape(head_count, depth)
    keys3 = keys.reshape(keys.shape[0], head_count, depth)
    scores = jnp.einsum("hd,shd->hs", query2, keys3, preferred_element_type=jnp.float32)
    scores = scores * depth ** (-0.5) + score_offset[:, None]
    remain = jax.nn.log_sigmoid(-scores)
    within = lax.cumsum(remain, axis=1, reverse=True) - remain
    totals = jnp.sum(remain, axis=1)
    beyond = prefix(totals, "sp", add_terms, jnp.zeros_like(totals))
    sticks = jnp.exp(jax.nn.log_sigmoid(scores) + within + beyond[:, None]).astype(jnp.bfloat16)
    values3 = values.reshape(values.shape[0], head_count, depth)
    partial_value = jnp.einsum("hs,shd->hd", sticks, values3, preferred_element_type=jnp.float32)
    return lax.psum(partial_value, "sp")


def finish_read(mixed, output_gain, head_count):
    spread = jnp.mean(mixed * mixed, axis=-1, keepdims=True)
    result = mixed * lax.rsqrt(spread + EPSILON) * output_gain.reshape(head_count, -1)
    return result.reshape(-1).astype(jnp.bfloat16)


LANES = 128
VMEM_BYTES = 67043328
ROW_SLOTS = 8
MESH = pl.DeviceIdType.MESH


def chunk_rows(rows):
    return next(size for size in (2 * LANES, LANES) if rows % size == 0)


def fused_kernel(
    peers, x_hbm, gain_hbm, wk_hbm, wv_hbm, query_hbm, offset_hbm, out_gain_hbm,
    key_out, value_out, read_out,
    x, gain, wk, wv, query, offset, out_gain, kv, outbox, inbox,
    x_sem, in_sem, send_sem, recv_sem, own_sem, small_send, small_recv,
):
    rows = x.shape[0]
    width = wk.shape[1]
    chunk = kv.shape[3]
    chunks = rows // chunk
    depth = width // peers
    me = lax.axis_index("sp")
    f32, bf16 = jnp.float32, jnp.bfloat16

    def part(c):
        return pl.ds(c * chunk, chunk)

    loads = [
        pltpu.make_async_copy(src, dst, in_sem.at[i])
        for i, (src, dst) in enumerate(
            ((gain_hbm, gain), (wk_hbm, wk), (wv_hbm, wv), (query_hbm, query), (offset_hbm, offset), (out_gain_hbm, out_gain))
        )
    ]
    x_loads = [pltpu.make_async_copy(x_hbm.at[part(c), :], x.at[part(c), :], x_sem.at[c]) for c in range(chunks)]
    loads[0].start()
    x_loads[0].start()
    loads[1].start()
    loads[2].start()
    for copy in x_loads[1:] + loads[3:]:
        copy.start()

    barrier = pltpu.get_barrier_semaphore()
    others = [lax.rem(me + d, peers) for d in range(1, peers)]
    for peer in others:
        pl.semaphore_signal(barrier, inc=1, device_id={"sp": peer}, device_id_type=MESH)

    outs = (key_out, value_out)
    order = sorted(range(1, peers), key=lambda d: -min(d, peers - d))

    def send(kind, c, d):
        peer = lax.rem(me + d, peers)
        return pltpu.make_async_remote_copy(
            src_ref=kv.at[kind, c, pl.ds(pl.multiple_of(peer * depth, depth), depth), :],
            dst_ref=outs[kind].at[me, :, part(c)],
            send_sem=send_sem.at[kind, c, d - 1],
            recv_sem=recv_sem.at[kind, c, d - 1],
            device_id={"sp": peer},
            device_id_type=MESH,
        )

    def keep(kind, c):
        return pltpu.make_async_copy(
            kv.at[kind, c, pl.ds(pl.multiple_of(me * depth, depth), depth), :],
            outs[kind].at[me, :, part(c)],
            own_sem.at[kind, c],
        )

    def send_all(c):
        for d in order:
            send(0, c, d).start()
            send(1, c, d).start()
        keep(0, c).start()
        keep(1, c).start()

    loads[0].wait()
    gain_row = gain[...].reshape(1, -1)
    for c in range(chunks):
        x_loads[c].wait()
        x32 = x[part(c), :].astype(f32)
        mean_square = jnp.mean(x32 * x32, axis=-1, keepdims=True)
        normed = (x32 * lax.rsqrt(mean_square + EPSILON) * gain_row).astype(bf16)
        for kind, weight in ((0, wk), (1, wv)):
            if c == 0:
                loads[1 + kind].wait()
            product = jnp.dot(normed, weight[...], preferred_element_type=f32)
            kv[kind, c] = product.T.astype(bf16)
        if c == 0:
            pl.semaphore_wait(barrier, peers - 1)
        if c < chunks - 1:
            send_all(c)

    for copy in loads[3:]:
        copy.wait()
    head_of = lax.broadcasted_iota(jnp.int32, (ROW_SLOTS, width), 1) // depth
    mine = head_of == lax.broadcasted_iota(jnp.int32, (ROW_SLOTS, width), 0)
    query_rows = jnp.where(mine, query[...].astype(f32).reshape(1, -1), 0.0).astype(bf16)
    slot = lax.broadcasted_iota(jnp.int32, (ROW_SLOTS, 1), 0)
    shift = jnp.zeros((ROW_SLOTS, 1), f32)
    for h in range(peers):
        shift = jnp.where(slot == h, offset[h], shift)
    scores = [
        jnp.dot(query_rows, kv[0, c], preferred_element_type=f32) * depth ** (-0.5) + shift for c in range(chunks)
    ]
    tiles = [s[:, t * LANES:(t + 1) * LANES] for s in scores for t in range(chunk // LANES)]
    stacked = jnp.concatenate(tiles, axis=0)
    tail = jnp.log1p(jnp.exp(-jnp.abs(stacked)))
    remain = -jnp.maximum(stacked, 0.0) - tail
    later = lax.broadcasted_iota(jnp.int32, (LANES, LANES), 0) > lax.broadcasted_iota(jnp.int32, (LANES, LANES), 1)
    within = jnp.dot(remain, later.astype(f32), precision=lax.Precision.HIGHEST, preferred_element_type=f32)
    sums = jnp.sum(remain, axis=1, keepdims=True)
    running = jnp.zeros((ROW_SLOTS, 1), f32)
    beyond = [None] * len(tiles)
    for t in reversed(range(len(tiles))):
        beyond[t] = running
        running = running + sums[t * ROW_SLOTS:(t + 1) * ROW_SLOTS]
    sticks = jnp.exp(jnp.minimum(stacked, 0.0) - tail + within + jnp.concatenate(beyond, axis=0)).astype(bf16)
    partial = jnp.zeros((ROW_SLOTS, width), f32)
    per = chunk // LANES
    for c in range(chunks):
        block = jnp.concatenate(
            [sticks[(c * per + t) * ROW_SLOTS:(c * per + t + 1) * ROW_SLOTS] for t in range(per)], axis=1
        )
        partial = partial + lax.dot_general(
            block, kv[1, c], (((1,), (1,)), ((), ())), preferred_element_type=f32
        )
    zeros = jnp.zeros((ROW_SLOTS, width), f32)
    outbox[0:1, :] = jnp.sum(jnp.where(mine, partial, zeros), axis=0, keepdims=True)
    outbox[1:2, :] = jnp.sum(jnp.where(mine, running, zeros), axis=0, keepdims=True)

    def post(d):
        return pltpu.make_async_remote_copy(
            src_ref=outbox,
            dst_ref=inbox.at[d],
            send_sem=small_send.at[d - 1],
            recv_sem=small_recv.at[d - 1],
            device_id={"sp": lax.rem(me + d, peers)},
            device_id_type=MESH,
        )

    for d in order:
        post(d).start()
    send_all(chunks - 1)

    for d in range(1, peers):
        post(d).wait_recv()
    totals, values = [outbox[1:2, :]], [outbox[0:1, :]]
    for d in range(1, peers):
        totals.append(inbox[d, 1:2, :])
        values.append(inbox[d, 0:1, :])
    places = [lax.rem(me - d + peers, peers) for d in range(peers)]
    mixed = jnp.zeros((1, width), f32)
    for d in range(peers):
        after = jnp.zeros((1, width), f32)
        for e in range(peers):
            if e != d:
                after = after + jnp.where(places[e] > places[d], totals[e], 0.0)
        mixed = mixed + values[d] * jnp.exp(after)
    spread = jnp.sum(jnp.where(mine, mixed * mixed, zeros), axis=1, keepdims=True) * (1.0 / depth)
    scale = jnp.sum(jnp.where(mine, lax.rsqrt(spread + EPSILON), zeros), axis=0, keepdims=True)
    read_out[...] = (mixed * scale * out_gain[...].reshape(1, -1)).astype(bf16).reshape(read_out.shape)

    for d in order:
        post(d).wait_send()
    for c in range(chunks):
        for kind in range(2):
            keep(kind, c).wait()
            for d in order:
                send(kind, c, d).wait()


def fused_body(prompt_rows, norm_gain, key_weight, value_weight, new_query, score_offset, output_gain):
    peers = lax.axis_size("sp")
    rows, features = prompt_rows.shape
    width = key_weight.shape[1]
    depth = width // peers
    chunk = chunk_rows(rows)
    chunks = rows // chunk
    f32, bf16 = jnp.float32, jnp.bfloat16
    vmem = pl.BlockSpec(memory_space=pltpu.VMEM)
    vmem_left = VMEM_BYTES - 2 * peers * depth * rows * 2 - 8192
    dma = pltpu.SemaphoreType.DMA
    cache = jax.ShapeDtypeStruct((peers, depth, rows), bf16)
    keys, values, read = pl.pallas_call(
        functools.partial(fused_kernel, peers),
        out_shape=(cache, cache, jax.ShapeDtypeStruct((width,), bf16)),
        in_specs=[pl.BlockSpec(memory_space=pltpu.HBM)] * 7,
        out_specs=(vmem, vmem, vmem),
        scratch_shapes=[
            pltpu.VMEM((rows, features), bf16),
            pltpu.VMEM((features,), f32),
            pltpu.VMEM((features, width), bf16),
            pltpu.VMEM((features, width), bf16),
            pltpu.VMEM((width,), bf16),
            pltpu.SMEM(score_offset.shape, f32),
            pltpu.VMEM((width,), f32),
            pltpu.VMEM((2, chunks, width, chunk), bf16),
            pltpu.VMEM((2, width), f32),
            pltpu.VMEM((peers, 2, width), f32),
            dma((chunks,)),
            dma((6,)),
            dma((2, chunks, peers - 1)),
            dma((2, chunks, peers - 1)),
            dma((2, chunks)),
            dma((peers - 1,)),
            dma((peers - 1,)),
        ],
        compiler_params=pltpu.CompilerParams(
            collective_id=0, has_side_effects=True, vmem_limit_bytes=vmem_left
        ),
        name="fused_cache_read",
    )(prompt_rows, norm_gain, key_weight, value_weight, new_query, score_offset, output_gain)

    def arrange(cache):
        return jnp.swapaxes(cache, 1, 2).reshape(1, 1, peers, rows, depth)

    return (arrange(keys), arrange(values), read)


def plain_body(prompt_rows, norm_gain, key_weight, value_weight, new_query, score_offset, output_gain):
    head_count = score_offset.shape[0]
    keys_here, values_here = project_rows(prompt_rows, norm_gain, key_weight, value_weight)
    keys_all, values_all = cache_layout(keys_here, values_here, head_count)
    local_keys, local_values = project_rows(prompt_rows, norm_gain, key_weight, value_weight)
    mixed = read_early(new_query, local_keys, local_values, score_offset)
    return (keys_all, values_all, finish_read(mixed, output_gain, head_count))


def body(prompt_rows, norm_gain, key_weight, value_weight, new_query, score_offset, output_gain):
    arguments = (prompt_rows, norm_gain, key_weight, value_weight, new_query, score_offset, output_gain)
    heads, devices = score_offset.shape[0], lax.axis_size("sp")
    rows, depth = prompt_rows.shape[0], key_weight.shape[1] // heads
    if heads == devices and heads <= 8 and rows % LANES == 0 and depth % 16 == 0 and key_weight.shape[1] % LANES == 0:
        return fused_body(*arguments)
    return plain_body(*arguments)


def solution(mesh):
    in_specs = (
        P(("grp", "sp"), None),
        P(),
        P(None, "tp"),
        P(None, "tp"),
        P(("grp", "tp")),
        P("tp"),
        P("tp"),
    )
    out_specs = (
        P(("grp", "tp"), "sp", None, None, None),
        P(("grp", "tp"), "sp", None, None, None),
        P(("grp", "tp")),
    )
    return jax.shard_map(body, mesh=mesh, in_specs=in_specs, out_specs=out_specs, check_vma=False)
```

```python
import functools

import jax
import jax.numpy as jnp
from jax import lax
from jax.experimental import pallas as pl
from jax.experimental.pallas import tpu as pltpu
from jax.sharding import PartitionSpec as P

EPSILON = 1e-06


def prefix(value, axis, combine, identity):
    peers, position = (lax.axis_size(axis), lax.axis_index(axis))
    everything = lax.all_gather(value, axis)
    start = jnp.broadcast_to(jnp.asarray(identity, value.dtype), value.shape)

    def hop(k, before):
        at = peers - 1 - k
        reached = at > position
        new = combine(before, everything[at])
        return jnp.where(reached, new, before)

    return lax.fori_loop(0, peers, hop, start)


def normalize(rows, norm_gain):
    rows32 = rows.astype(jnp.float32)
    mean_square = jnp.mean(rows32 * rows32, axis=-1, keepdims=True)
    return (rows32 * lax.rsqrt(mean_square + EPSILON) * norm_gain).astype(jnp.bfloat16)


def project_rows(rows, norm_gain, key_weight, value_weight):
    normed = normalize(rows, norm_gain)
    keys = jnp.dot(normed, key_weight, preferred_element_type=jnp.float32).astype(jnp.bfloat16)
    values = jnp.dot(normed, value_weight, preferred_element_type=jnp.float32).astype(jnp.bfloat16)
    return (keys, values)


def cache_layout(keys, values, head_count):
    devices = lax.axis_size("sp")
    subs = devices // head_count
    depth = keys.shape[1] // head_count
    rows = keys.shape[0] // subs

    def arrange(cache):
        split = cache.reshape(subs, rows, head_count, depth)
        return jnp.transpose(split, (2, 0, 1, 3)).reshape(devices, 1, rows, depth)

    moved_keys, moved_values = (
        lax.all_to_all(arrange(keys), "sp", split_axis=0, concat_axis=1, tiled=True),
        lax.all_to_all(arrange(values), "sp", split_axis=0, concat_axis=1, tiled=True),
    )
    target = (1, 1, devices, rows, depth)
    return (moved_keys.reshape(target), moved_values.reshape(target))


def add_terms(first_part, second_part):
    return first_part + second_part


def read_early(new_query, keys, values, score_offset):
    head_count = score_offset.shape[0]
    depth = keys.shape[1] // head_count
    query2 = new_query.reshape(head_count, depth)
    keys3 = keys.reshape(keys.shape[0], head_count, depth)
    scores = jnp.einsum("hd,shd->hs", query2, keys3, preferred_element_type=jnp.float32)
    scores = scores * depth ** (-0.5) + score_offset[:, None]
    remain = jax.nn.log_sigmoid(-scores)
    within = lax.cumsum(remain, axis=1, reverse=True) - remain
    totals = jnp.sum(remain, axis=1)
    beyond = prefix(totals, "sp", add_terms, jnp.zeros_like(totals))
    sticks = jnp.exp(jax.nn.log_sigmoid(scores) + within + beyond[:, None]).astype(jnp.bfloat16)
    values3 = values.reshape(values.shape[0], head_count, depth)
    partial_value = jnp.einsum("hs,shd->hd", sticks, values3, preferred_element_type=jnp.float32)
    return lax.psum(partial_value, "sp")


def finish_read(mixed, output_gain, head_count):
    spread = jnp.mean(mixed * mixed, axis=-1, keepdims=True)
    result = mixed * lax.rsqrt(spread + EPSILON) * output_gain.reshape(head_count, -1)
    return result.reshape(-1).astype(jnp.bfloat16)


LANES = 128
ROW_SLOTS = 8
VMEM_LIMIT = 40 * 1024 * 1024
MESH = pl.DeviceIdType.MESH


def row_chunks(rows):
    sizes, left = [], rows
    while left:
        size = min((len(sizes) + 1) * LANES, left)
        sizes.append(size)
        left -= size
    return [(sum(sizes[:i]), size) for i, size in enumerate(sizes)]


def fused_kernel(
    peers, x_hbm, gain_hbm, wk_hbm, wv_hbm, query_hbm, offset_hbm, out_gain_hbm,
    key_out, value_out, read_out,
    x, gain, wk, wv, query, offset, out_gain, kv, outbox, inbox,
    x_sem, in_sem, send_sem, recv_sem, own_sem, small_send, small_recv,
):
    rows = x.shape[0]
    width = wk.shape[1]
    spans = row_chunks(rows)
    chunks = len(spans)
    depth = width // peers
    me = lax.axis_index("sp")
    f32, bf16 = jnp.float32, jnp.bfloat16

    def part(c):
        return pl.ds(*spans[c])

    loads = [
        pltpu.make_async_copy(src, dst, in_sem.at[i])
        for i, (src, dst) in enumerate(
            ((gain_hbm, gain), (wk_hbm, wk), (wv_hbm, wv), (query_hbm, query), (offset_hbm, offset), (out_gain_hbm, out_gain))
        )
    ]
    x_loads = [pltpu.make_async_copy(x_hbm.at[part(c), :], x.at[part(c), :], x_sem.at[c]) for c in range(chunks)]
    loads[0].start()
    x_loads[0].start()
    loads[1].start()
    loads[2].start()
    for copy in x_loads[1:] + loads[3:]:
        copy.start()

    barrier = pltpu.get_barrier_semaphore()
    others = [lax.rem(me + d, peers) for d in range(1, peers)]
    for peer in others:
        pl.semaphore_signal(barrier, inc=1, device_id={"sp": peer}, device_id_type=MESH)

    outs = (key_out, value_out)
    left_half = 1 - (2 * me) // peers
    targets = []
    for j in range(peers - 1):
        down, up = peers - 1 - j, j
        down = down - (1 - (down - me + peers - 1) // peers)
        up = up + (1 - (me - up + peers - 1) // peers)
        targets.append(left_half * down + (1 - left_half) * up)

    def head_rows(place):
        return pl.ds(pl.multiple_of(place * depth, depth), depth)

    def send(kind, c, j):
        return pltpu.make_async_remote_copy(
            src_ref=kv.at[kind, head_rows(targets[j]), part(c)],
            dst_ref=outs[kind].at[me, :, part(c)],
            send_sem=send_sem.at[kind, c, j],
            recv_sem=recv_sem.at[kind, c, me],
            device_id={"sp": targets[j]},
            device_id_type=MESH,
        )

    def arrival(kind, c, j):
        return pltpu.make_async_remote_copy(
            src_ref=kv.at[kind, head_rows(targets[j]), part(c)],
            dst_ref=outs[kind].at[targets[j], :, part(c)],
            send_sem=send_sem.at[kind, c, j],
            recv_sem=recv_sem.at[kind, c, targets[j]],
            device_id={"sp": targets[j]},
            device_id_type=MESH,
        )

    def keep(kind, c):
        return pltpu.make_async_copy(
            kv.at[kind, head_rows(me), part(c)], outs[kind].at[me, :, part(c)], own_sem.at[kind, c]
        )

    def send_all(c, kinds=(0, 1)):
        slots = range(peers - 1) if c < chunks - 1 else reversed(range(peers - 1))
        for j in slots:
            for kind in kinds:
                send(kind, c, j).start()
        for kind in kinds:
            keep(kind, c).start()

    loads[0].wait()
    gain_row = gain[...].reshape(1, -1)
    for c in range(chunks):
        x_loads[c].wait()
        x32 = x[part(c), :].astype(f32)
        mean_square = jnp.mean(x32 * x32, axis=-1, keepdims=True)
        normed = (x32 * lax.rsqrt(mean_square + EPSILON) * gain_row).astype(bf16)
        for kind, weight in ((0, wk), (1, wv)):
            if c == 0:
                loads[1 + kind].wait()
            product = jnp.dot(normed, weight[...], preferred_element_type=f32)
            kv[kind, :, part(c)] = product.T.astype(bf16)
            if c == 0 and kind == 0:
                pl.semaphore_wait(barrier, peers - 1)
            if c < chunks - 1:
                send_all(c, (kind,))

    for copy in loads[3:]:
        copy.wait()
    head_of = lax.broadcasted_iota(jnp.int32, (ROW_SLOTS, width), 1) // depth
    mine = head_of == lax.broadcasted_iota(jnp.int32, (ROW_SLOTS, width), 0)
    query_rows = jnp.where(mine, query[...].astype(f32).reshape(1, -1), 0.0).astype(bf16)
    slot = lax.broadcasted_iota(jnp.int32, (ROW_SLOTS, 1), 0)
    shift = jnp.zeros((ROW_SLOTS, 1), f32)
    for h in range(peers):
        shift = jnp.where(slot == h, offset[h], shift)
    scores = jnp.dot(query_rows, kv[0], preferred_element_type=f32) * depth ** (-0.5) + shift
    tiles = [scores[:, t * LANES:(t + 1) * LANES] for t in range(rows // LANES)]
    stacked = jnp.concatenate(tiles, axis=0)
    tail = jnp.log1p(jnp.exp(-jnp.abs(stacked)))
    remain = -jnp.maximum(stacked, 0.0) - tail
    later = lax.broadcasted_iota(jnp.int32, (LANES, LANES), 0) > lax.broadcasted_iota(jnp.int32, (LANES, LANES), 1)
    within = jnp.dot(remain, later.astype(f32), precision=lax.Precision.HIGHEST, preferred_element_type=f32)
    sums = jnp.sum(remain, axis=1, keepdims=True)
    running = jnp.zeros((ROW_SLOTS, 1), f32)
    beyond = [None] * len(tiles)
    for t in reversed(range(len(tiles))):
        beyond[t] = running
        running = running + sums[t * ROW_SLOTS:(t + 1) * ROW_SLOTS]
    sticks = jnp.exp(jnp.minimum(stacked, 0.0) - tail + within + jnp.concatenate(beyond, axis=0)).astype(bf16)
    sticks = jnp.concatenate([sticks[t * ROW_SLOTS:(t + 1) * ROW_SLOTS] for t in range(len(tiles))], axis=1)
    partial = lax.dot_general(sticks, kv[1], (((1,), (1,)), ((), ())), preferred_element_type=f32)
    zeros = jnp.zeros((ROW_SLOTS, width), f32)
    outbox[0:1, :] = jnp.sum(jnp.where(mine, partial, zeros), axis=0, keepdims=True)
    outbox[1:2, :] = jnp.sum(jnp.where(mine, running, zeros), axis=0, keepdims=True)

    def post(d):
        return pltpu.make_async_remote_copy(
            src_ref=outbox,
            dst_ref=inbox.at[d],
            send_sem=small_send.at[d - 1],
            recv_sem=small_recv.at[d - 1],
            device_id={"sp": lax.rem(me + d, peers)},
            device_id_type=MESH,
        )

    for d in range(1, peers):
        post(d).start()
    send_all(chunks - 1)

    for d in range(1, peers):
        post(d).wait_recv()
    totals, values = [outbox[1:2, :]], [outbox[0:1, :]]
    for d in range(1, peers):
        totals.append(inbox[d, 1:2, :])
        values.append(inbox[d, 0:1, :])
    places = [lax.rem(me - d + peers, peers) for d in range(peers)]
    mixed = jnp.zeros((1, width), f32)
    for d in range(peers):
        after = jnp.zeros((1, width), f32)
        for e in range(peers):
            if e != d:
                after = after + jnp.where(places[e] > places[d], totals[e], 0.0)
        mixed = mixed + values[d] * jnp.exp(after)
    spread = jnp.sum(jnp.where(mine, mixed * mixed, zeros), axis=1, keepdims=True) * (1.0 / depth)
    scale = jnp.sum(jnp.where(mine, lax.rsqrt(spread + EPSILON), zeros), axis=0, keepdims=True)
    read_out[...] = (mixed * scale * out_gain[...].reshape(1, -1)).astype(bf16).reshape(read_out.shape)

    for d in range(1, peers):
        post(d).wait_send()
    for c in range(chunks):
        for kind in range(2):
            keep(kind, c).wait()
            for j in range(peers - 1):
                send(kind, c, j).wait_send()
                arrival(kind, c, j).wait_recv()


def write_kernel(sources, targets, sems):
    copies = [pltpu.make_async_copy(src, dst, sems.at[i]) for i, (src, dst) in enumerate(zip(sources, targets))]
    for copy in copies:
        copy.start()
    for copy in copies:
        copy.wait()


def write_out(*arrays):
    count = len(arrays)

    def kernel(*refs):
        write_kernel(refs[:count], refs[count:2 * count], refs[2 * count])

    return pl.pallas_call(
        kernel,
        out_shape=tuple(jax.ShapeDtypeStruct(a.shape, a.dtype) for a in arrays),
        in_specs=[pl.BlockSpec(memory_space=pltpu.VMEM)] * count,
        out_specs=(pl.BlockSpec(memory_space=pltpu.HBM),) * count,
        scratch_shapes=[pltpu.SemaphoreType.DMA((count,))],
        compiler_params=pltpu.CompilerParams(vmem_limit_bytes=1024 * 1024),
        name="write_out",
    )(*arrays)


def fused_body(*arguments):
    prompt_rows, norm_gain, key_weight, value_weight, new_query, score_offset, output_gain = arguments
    peers = lax.axis_size("sp")
    rows, features = prompt_rows.shape
    width = key_weight.shape[1]
    depth = width // peers
    chunks = len(row_chunks(rows))
    f32, bf16 = jnp.float32, jnp.bfloat16
    vmem = pl.BlockSpec(memory_space=pltpu.VMEM)

    dma = pltpu.SemaphoreType.DMA
    cache = jax.ShapeDtypeStruct((peers, depth, rows), bf16)
    keys, values, read = pl.pallas_call(
        functools.partial(fused_kernel, peers),
        out_shape=(cache, cache, jax.ShapeDtypeStruct((width,), bf16)),
        in_specs=[pl.BlockSpec(memory_space=pltpu.HBM)] * 7,
        out_specs=(vmem, vmem, vmem),
        scratch_shapes=[
            pltpu.VMEM((rows, features), bf16),
            pltpu.VMEM((features,), f32),
            pltpu.VMEM((features, width), bf16),
            pltpu.VMEM((features, width), bf16),
            pltpu.VMEM((width,), bf16),
            pltpu.SMEM(score_offset.shape, f32),
            pltpu.VMEM((width,), f32),
            pltpu.VMEM((2, width, rows), bf16),
            pltpu.VMEM((2, width), f32),
            pltpu.VMEM((peers, 2, width), f32),
            dma((chunks,)),
            dma((6,)),
            dma((2, chunks, peers - 1)),
            dma((2, chunks, peers)),
            dma((2, chunks)),
            dma((peers - 1,)),
            dma((peers - 1,)),
        ],
        compiler_params=pltpu.CompilerParams(
            collective_id=0, has_side_effects=True, vmem_limit_bytes=VMEM_LIMIT
        ),
        name="fused_cache_read",
    )(*[pltpu.with_memory_space_constraint(argument, pltpu.HBM) for argument in arguments])

    keys, values, read = write_out(keys, values, read)

    def arrange(cache):
        return jnp.swapaxes(cache, 1, 2).reshape(1, 1, peers, rows, depth)

    return (arrange(keys), arrange(values), read)


def plain_body(prompt_rows, norm_gain, key_weight, value_weight, new_query, score_offset, output_gain):
    head_count = score_offset.shape[0]
    keys_here, values_here = project_rows(prompt_rows, norm_gain, key_weight, value_weight)
    keys_all, values_all = cache_layout(keys_here, values_here, head_count)
    local_keys, local_values = project_rows(prompt_rows, norm_gain, key_weight, value_weight)
    mixed = read_early(new_query, local_keys, local_values, score_offset)
    return (keys_all, values_all, finish_read(mixed, output_gain, head_count))


def body(prompt_rows, norm_gain, key_weight, value_weight, new_query, score_offset, output_gain):
    arguments = (prompt_rows, norm_gain, key_weight, value_weight, new_query, score_offset, output_gain)
    heads, devices = score_offset.shape[0], lax.axis_size("sp")
    rows, depth = prompt_rows.shape[0], key_weight.shape[1] // heads
    if heads == devices and heads <= 8 and rows % LANES == 0 and depth % 16 == 0 and key_weight.shape[1] % LANES == 0:
        return fused_body(*arguments)
    return plain_body(*arguments)


def solution(mesh):
    in_specs = (
        P(("grp", "sp"), None),
        P(),
        P(None, "tp"),
        P(None, "tp"),
        P(("grp", "tp")),
        P("tp"),
        P("tp"),
    )
    out_specs = (
        P(("grp", "tp"), "sp", None, None, None),
        P(("grp", "tp"), "sp", None, None, None),
        P(("grp", "tp")),
    )
    return jax.shard_map(body, mesh=mesh, in_specs=in_specs, out_specs=out_specs, check_vma=False)
```

```python
import functools

import jax
import jax.numpy as jnp
from jax import lax
from jax.experimental import pallas as pl
from jax.experimental.pallas import tpu as pltpu
from jax.sharding import PartitionSpec as P

EPSILON = 1e-06


def prefix(value, axis, combine, identity):
    peers, position = (lax.axis_size(axis), lax.axis_index(axis))
    everything = lax.all_gather(value, axis)
    start = jnp.broadcast_to(jnp.asarray(identity, value.dtype), value.shape)

    def hop(k, before):
        at = peers - 1 - k
        reached = at > position
        new = combine(before, everything[at])
        return jnp.where(reached, new, before)

    return lax.fori_loop(0, peers, hop, start)


def normalize(rows, norm_gain):
    rows32 = rows.astype(jnp.float32)
    mean_square = jnp.mean(rows32 * rows32, axis=-1, keepdims=True)
    return (rows32 * lax.rsqrt(mean_square + EPSILON) * norm_gain).astype(jnp.bfloat16)


def project_rows(rows, norm_gain, key_weight, value_weight):
    normed = normalize(rows, norm_gain)
    keys = jnp.dot(normed, key_weight, preferred_element_type=jnp.float32).astype(jnp.bfloat16)
    values = jnp.dot(normed, value_weight, preferred_element_type=jnp.float32).astype(jnp.bfloat16)
    return (keys, values)


def cache_layout(keys, values, head_count):
    devices = lax.axis_size("sp")
    subs = devices // head_count
    depth = keys.shape[1] // head_count
    rows = keys.shape[0] // subs

    def arrange(cache):
        split = cache.reshape(subs, rows, head_count, depth)
        return jnp.transpose(split, (2, 0, 1, 3)).reshape(devices, 1, rows, depth)

    moved_keys, moved_values = (
        lax.all_to_all(arrange(keys), "sp", split_axis=0, concat_axis=1, tiled=True),
        lax.all_to_all(arrange(values), "sp", split_axis=0, concat_axis=1, tiled=True),
    )
    target = (1, 1, devices, rows, depth)
    return (moved_keys.reshape(target), moved_values.reshape(target))


def add_terms(first_part, second_part):
    return first_part + second_part


def read_early(new_query, keys, values, score_offset):
    head_count = score_offset.shape[0]
    depth = keys.shape[1] // head_count
    query2 = new_query.reshape(head_count, depth)
    keys3 = keys.reshape(keys.shape[0], head_count, depth)
    scores = jnp.einsum("hd,shd->hs", query2, keys3, preferred_element_type=jnp.float32)
    scores = scores * depth ** (-0.5) + score_offset[:, None]
    remain = jax.nn.log_sigmoid(-scores)
    within = lax.cumsum(remain, axis=1, reverse=True) - remain
    totals = jnp.sum(remain, axis=1)
    beyond = prefix(totals, "sp", add_terms, jnp.zeros_like(totals))
    sticks = jnp.exp(jax.nn.log_sigmoid(scores) + within + beyond[:, None]).astype(jnp.bfloat16)
    values3 = values.reshape(values.shape[0], head_count, depth)
    partial_value = jnp.einsum("hs,shd->hd", sticks, values3, preferred_element_type=jnp.float32)
    return lax.psum(partial_value, "sp")


def finish_read(mixed, output_gain, head_count):
    spread = jnp.mean(mixed * mixed, axis=-1, keepdims=True)
    result = mixed * lax.rsqrt(spread + EPSILON) * output_gain.reshape(head_count, -1)
    return result.reshape(-1).astype(jnp.bfloat16)


LANES = 128
ROW_SLOTS = 8
VMEM_LIMIT = 40 * 1024 * 1024
MESH = pl.DeviceIdType.MESH


def row_chunks(rows):
    sizes, left = [], rows
    while left:
        size = LANES if len(sizes) < 2 else left
        sizes.append(size)
        left -= size
    return [(sum(sizes[:i]), size) for i, size in enumerate(sizes)]


def fused_kernel(
    peers, x_hbm, gain_hbm, wk_hbm, wv_hbm, query_hbm, offset_hbm, out_gain_hbm,
    key_out, value_out, read_out,
    x, gain, wk, wv, query, offset, out_gain, kv, outbox, inbox,
    x_sem, in_sem, send_sem, recv_sem, own_sem, small_send, small_recv,
):
    rows = x.shape[0]
    width = wk.shape[1]
    spans = row_chunks(rows)
    chunks = len(spans)
    depth = width // peers
    me = lax.axis_index("sp")
    f32, bf16 = jnp.float32, jnp.bfloat16

    barrier = pltpu.get_barrier_semaphore()
    others = [lax.rem(me + d, peers) for d in range(1, peers)]
    for peer in others:
        pl.semaphore_signal(barrier, inc=1, device_id={"sp": peer}, device_id_type=MESH)

    def part(c):
        return pl.ds(*spans[c])

    loads = [
        pltpu.make_async_copy(src, dst, in_sem.at[i])
        for i, (src, dst) in enumerate(
            ((gain_hbm, gain), (wk_hbm, wk), (wv_hbm, wv), (query_hbm, query), (offset_hbm, offset), (out_gain_hbm, out_gain))
        )
    ]
    x_loads = [pltpu.make_async_copy(x_hbm.at[part(c), :], x.at[part(c), :], x_sem.at[c]) for c in range(chunks)]
    for copy in (loads[1], x_loads[0], loads[0], loads[2]):
        copy.start()

    outs = (key_out, value_out)
    left_half = 1 - (2 * me) // peers
    targets = []
    for j in range(peers - 1):
        down, up = peers - 1 - j, j
        down = down - (1 - (down - me + peers - 1) // peers)
        up = up + (1 - (me - up + peers - 1) // peers)
        targets.append(left_half * down + (1 - left_half) * up)

    def head_rows(place):
        return pl.ds(pl.multiple_of(place * depth, depth), depth)

    def send(kind, c, j):
        return pltpu.make_async_remote_copy(
            src_ref=kv.at[kind, head_rows(targets[j]), part(c)],
            dst_ref=outs[kind].at[me, :, part(c)],
            send_sem=send_sem.at[kind, c, j],
            recv_sem=recv_sem.at[kind, c, me],
            device_id={"sp": targets[j]},
            device_id_type=MESH,
        )

    def arrival(kind, c, j):
        return pltpu.make_async_remote_copy(
            src_ref=kv.at[kind, head_rows(targets[j]), part(c)],
            dst_ref=outs[kind].at[targets[j], :, part(c)],
            send_sem=send_sem.at[kind, c, j],
            recv_sem=recv_sem.at[kind, c, targets[j]],
            device_id={"sp": targets[j]},
            device_id_type=MESH,
        )

    def keep(kind, c):
        return pltpu.make_async_copy(
            kv.at[kind, head_rows(me), part(c)], outs[kind].at[me, :, part(c)], own_sem.at[kind, c]
        )

    def send_all(c, kinds=(0, 1)):
        turn = 0 if c < chunks - 1 else peers // 2
        for j in [(turn + i) % (peers - 1) for i in range(peers - 1)]:
            for kind in kinds:
                send(kind, c, j).start()
        for kind in kinds:
            keep(kind, c).start()

    loads[0].wait()
    gain_row = gain[...].reshape(1, -1)
    for c in range(chunks):
        x_loads[c].wait()
        if c == 0:
            for copy in x_loads[1:] + loads[3:]:
                copy.start()
        x32 = x[part(c), :].astype(f32)
        mean_square = jnp.mean(x32 * x32, axis=-1, keepdims=True)
        normed = (x32 * lax.rsqrt(mean_square + EPSILON) * gain_row).astype(bf16)
        for kind, weight in ((0, wk), (1, wv)):
            if c == 0:
                loads[1 + kind].wait()
            product = jnp.dot(normed, weight[...], preferred_element_type=f32)
            kv[kind, :, part(c)] = product.T.astype(bf16)
            if c == 0 and kind == 0:
                pl.semaphore_wait(barrier, peers - 1)
            if c < chunks - 1:
                send_all(c, (kind,))

    for copy in loads[3:]:
        copy.wait()
    head_of = lax.broadcasted_iota(jnp.int32, (ROW_SLOTS, width), 1) // depth
    mine = head_of == lax.broadcasted_iota(jnp.int32, (ROW_SLOTS, width), 0)
    query_rows = jnp.where(mine, query[...].astype(f32).reshape(1, -1), 0.0).astype(bf16)
    slot = lax.broadcasted_iota(jnp.int32, (ROW_SLOTS, 1), 0)
    shift = jnp.zeros((ROW_SLOTS, 1), f32)
    for h in range(peers):
        shift = jnp.where(slot == h, offset[h], shift)
    scores = jnp.dot(query_rows, kv[0], preferred_element_type=f32) * depth ** (-0.5) + shift
    tiles = [scores[:, t * LANES:(t + 1) * LANES] for t in range(rows // LANES)]
    stacked = jnp.concatenate(tiles, axis=0)
    tail = jnp.log1p(jnp.exp(-jnp.abs(stacked)))
    remain = -jnp.maximum(stacked, 0.0) - tail
    later = lax.broadcasted_iota(jnp.int32, (LANES, LANES), 0) > lax.broadcasted_iota(jnp.int32, (LANES, LANES), 1)
    within = jnp.dot(remain, later.astype(f32), precision=lax.Precision.HIGHEST, preferred_element_type=f32)
    sums = jnp.sum(remain, axis=1, keepdims=True)
    running = jnp.zeros((ROW_SLOTS, 1), f32)
    beyond = [None] * len(tiles)
    for t in reversed(range(len(tiles))):
        beyond[t] = running
        running = running + sums[t * ROW_SLOTS:(t + 1) * ROW_SLOTS]
    sticks = jnp.exp(jnp.minimum(stacked, 0.0) - tail + within + jnp.concatenate(beyond, axis=0)).astype(bf16)
    sticks = jnp.concatenate([sticks[t * ROW_SLOTS:(t + 1) * ROW_SLOTS] for t in range(len(tiles))], axis=1)
    partial = lax.dot_general(sticks, kv[1], (((1,), (1,)), ((), ())), preferred_element_type=f32)
    zeros = jnp.zeros((ROW_SLOTS, width), f32)
    outbox[0:1, :] = jnp.sum(jnp.where(mine, partial, zeros), axis=0, keepdims=True)
    outbox[1:2, :] = jnp.sum(jnp.where(mine, running, zeros), axis=0, keepdims=True)

    def post(d):
        return pltpu.make_async_remote_copy(
            src_ref=outbox,
            dst_ref=inbox.at[d],
            send_sem=small_send.at[d - 1],
            recv_sem=small_recv.at[d - 1],
            device_id={"sp": lax.rem(me + d, peers)},
            device_id_type=MESH,
        )

    for d in range(1, peers):
        post(d).start()
    send_all(chunks - 1)

    for d in range(1, peers):
        post(d).wait_recv()
    totals, values = [outbox[1:2, :]], [outbox[0:1, :]]
    for d in range(1, peers):
        totals.append(inbox[d, 1:2, :])
        values.append(inbox[d, 0:1, :])
    places = [lax.rem(me - d + peers, peers) for d in range(peers)]
    mixed = jnp.zeros((1, width), f32)
    for d in range(peers):
        after = jnp.zeros((1, width), f32)
        for e in range(peers):
            if e != d:
                after = after + jnp.where(places[e] > places[d], totals[e], 0.0)
        mixed = mixed + values[d] * jnp.exp(after)
    spread = jnp.sum(jnp.where(mine, mixed * mixed, zeros), axis=1, keepdims=True) * (1.0 / depth)
    scale = jnp.sum(jnp.where(mine, lax.rsqrt(spread + EPSILON), zeros), axis=0, keepdims=True)
    read_out[...] = (mixed * scale * out_gain[...].reshape(1, -1)).astype(bf16).reshape(read_out.shape)

    for d in range(1, peers):
        post(d).wait_send()
    for c in range(chunks):
        for kind in range(2):
            keep(kind, c).wait()
            for j in range(peers - 1):
                send(kind, c, j).wait_send()
                arrival(kind, c, j).wait_recv()


def write_kernel(sources, targets, sems):
    copies = [pltpu.make_async_copy(src, dst, sems.at[i]) for i, (src, dst) in enumerate(zip(sources, targets))]
    for copy in copies:
        copy.start()
    for copy in copies:
        copy.wait()


def write_out(*arrays):
    count = len(arrays)

    def kernel(*refs):
        write_kernel(refs[:count], refs[count:2 * count], refs[2 * count])

    return pl.pallas_call(
        kernel,
        out_shape=tuple(jax.ShapeDtypeStruct(a.shape, a.dtype) for a in arrays),
        in_specs=[pl.BlockSpec(memory_space=pltpu.VMEM)] * count,
        out_specs=(pl.BlockSpec(memory_space=pltpu.HBM),) * count,
        scratch_shapes=[pltpu.SemaphoreType.DMA((count,))],
        compiler_params=pltpu.CompilerParams(vmem_limit_bytes=1024 * 1024),
        name="write_out",
    )(*arrays)


def fused_body(*arguments):
    prompt_rows, norm_gain, key_weight, value_weight, new_query, score_offset, output_gain = arguments
    peers = lax.axis_size("sp")
    rows, features = prompt_rows.shape
    width = key_weight.shape[1]
    depth = width // peers
    chunks = len(row_chunks(rows))
    f32, bf16 = jnp.float32, jnp.bfloat16
    vmem = pl.BlockSpec(memory_space=pltpu.VMEM)

    dma = pltpu.SemaphoreType.DMA
    cache = jax.ShapeDtypeStruct((peers, depth, rows), bf16)
    keys, values, read = pl.pallas_call(
        functools.partial(fused_kernel, peers),
        out_shape=(cache, cache, jax.ShapeDtypeStruct((width,), bf16)),
        in_specs=[pl.BlockSpec(memory_space=pltpu.HBM)] * 7,
        out_specs=(vmem, vmem, vmem),
        scratch_shapes=[
            pltpu.VMEM((rows, features), bf16),
            pltpu.VMEM((features,), f32),
            pltpu.VMEM((features, width), bf16),
            pltpu.VMEM((features, width), bf16),
            pltpu.VMEM((width,), bf16),
            pltpu.SMEM(score_offset.shape, f32),
            pltpu.VMEM((width,), f32),
            pltpu.VMEM((2, width, rows), bf16),
            pltpu.VMEM((2, width), f32),
            pltpu.VMEM((peers, 2, width), f32),
            dma((chunks,)),
            dma((6,)),
            dma((2, chunks, peers - 1)),
            dma((2, chunks, peers)),
            dma((2, chunks)),
            dma((peers - 1,)),
            dma((peers - 1,)),
        ],
        compiler_params=pltpu.CompilerParams(
            collective_id=0, has_side_effects=True, vmem_limit_bytes=VMEM_LIMIT
        ),
        name="fused_cache_read",
    )(*[pltpu.with_memory_space_constraint(argument, pltpu.HBM) for argument in arguments])

    keys, values, read = write_out(keys, values, read)

    def arrange(cache):
        return jnp.swapaxes(cache, 1, 2).reshape(1, 1, peers, rows, depth)

    return (arrange(keys), arrange(values), read)


def plain_body(prompt_rows, norm_gain, key_weight, value_weight, new_query, score_offset, output_gain):
    head_count = score_offset.shape[0]
    keys_here, values_here = project_rows(prompt_rows, norm_gain, key_weight, value_weight)
    keys_all, values_all = cache_layout(keys_here, values_here, head_count)
    local_keys, local_values = project_rows(prompt_rows, norm_gain, key_weight, value_weight)
    mixed = read_early(new_query, local_keys, local_values, score_offset)
    return (keys_all, values_all, finish_read(mixed, output_gain, head_count))


def body(prompt_rows, norm_gain, key_weight, value_weight, new_query, score_offset, output_gain):
    arguments = (prompt_rows, norm_gain, key_weight, value_weight, new_query, score_offset, output_gain)
    heads, devices = score_offset.shape[0], lax.axis_size("sp")
    rows, depth = prompt_rows.shape[0], key_weight.shape[1] // heads
    if heads == devices and heads <= 8 and rows % LANES == 0 and depth % 16 == 0 and key_weight.shape[1] % LANES == 0:
        return fused_body(*arguments)
    return plain_body(*arguments)


def solution(mesh):
    in_specs = (
        P(("grp", "sp"), None),
        P(),
        P(None, "tp"),
        P(None, "tp"),
        P(("grp", "tp")),
        P("tp"),
        P("tp"),
    )
    out_specs = (
        P(("grp", "tp"), "sp", None, None, None),
        P(("grp", "tp"), "sp", None, None, None),
        P(("grp", "tp")),
    )
    return jax.shard_map(body, mesh=mesh, in_specs=in_specs, out_specs=out_specs, check_vma=False)
```

```python
import functools

import jax
import jax.numpy as jnp
from jax import lax
from jax.experimental import pallas as pl
from jax.experimental.pallas import tpu as pltpu
from jax.sharding import PartitionSpec as P

EPSILON = 1e-06


def prefix(value, axis, combine, identity):
    peers, position = (lax.axis_size(axis), lax.axis_index(axis))
    everything = lax.all_gather(value, axis)
    start = jnp.broadcast_to(jnp.asarray(identity, value.dtype), value.shape)

    def hop(k, before):
        at = peers - 1 - k
        reached = at > position
        new = combine(before, everything[at])
        return jnp.where(reached, new, before)

    return lax.fori_loop(0, peers, hop, start)


def normalize(rows, norm_gain):
    rows32 = rows.astype(jnp.float32)
    mean_square = jnp.mean(rows32 * rows32, axis=-1, keepdims=True)
    return (rows32 * lax.rsqrt(mean_square + EPSILON) * norm_gain).astype(jnp.bfloat16)


def project_rows(rows, norm_gain, key_weight, value_weight):
    normed = normalize(rows, norm_gain)
    keys = jnp.dot(normed, key_weight, preferred_element_type=jnp.float32).astype(jnp.bfloat16)
    values = jnp.dot(normed, value_weight, preferred_element_type=jnp.float32).astype(jnp.bfloat16)
    return (keys, values)


def cache_layout(keys, values, head_count):
    devices = lax.axis_size("sp")
    subs = devices // head_count
    depth = keys.shape[1] // head_count
    rows = keys.shape[0] // subs

    def arrange(cache):
        split = cache.reshape(subs, rows, head_count, depth)
        return jnp.transpose(split, (2, 0, 1, 3)).reshape(devices, 1, rows, depth)

    moved_keys, moved_values = (
        lax.all_to_all(arrange(keys), "sp", split_axis=0, concat_axis=1, tiled=True),
        lax.all_to_all(arrange(values), "sp", split_axis=0, concat_axis=1, tiled=True),
    )
    target = (1, 1, devices, rows, depth)
    return (moved_keys.reshape(target), moved_values.reshape(target))


def add_terms(first_part, second_part):
    return first_part + second_part


def read_early(new_query, keys, values, score_offset):
    head_count = score_offset.shape[0]
    depth = keys.shape[1] // head_count
    query2 = new_query.reshape(head_count, depth)
    keys3 = keys.reshape(keys.shape[0], head_count, depth)
    scores = jnp.einsum("hd,shd->hs", query2, keys3, preferred_element_type=jnp.float32)
    scores = scores * depth ** (-0.5) + score_offset[:, None]
    remain = jax.nn.log_sigmoid(-scores)
    within = lax.cumsum(remain, axis=1, reverse=True) - remain
    totals = jnp.sum(remain, axis=1)
    beyond = prefix(totals, "sp", add_terms, jnp.zeros_like(totals))
    sticks = jnp.exp(jax.nn.log_sigmoid(scores) + within + beyond[:, None]).astype(jnp.bfloat16)
    values3 = values.reshape(values.shape[0], head_count, depth)
    partial_value = jnp.einsum("hs,shd->hd", sticks, values3, preferred_element_type=jnp.float32)
    return lax.psum(partial_value, "sp")


def finish_read(mixed, output_gain, head_count):
    spread = jnp.mean(mixed * mixed, axis=-1, keepdims=True)
    result = mixed * lax.rsqrt(spread + EPSILON) * output_gain.reshape(head_count, -1)
    return result.reshape(-1).astype(jnp.bfloat16)


LANES = 128
ROW_SLOTS = 8
VMEM_LIMIT = 40 * 1024 * 1024
MESH = pl.DeviceIdType.MESH


def row_chunks(rows):
    sizes, left = [], rows
    while left:
        size = LANES if not sizes else left
        sizes.append(size)
        left -= size
    return [(sum(sizes[:i]), size) for i, size in enumerate(sizes)]


def fused_kernel(
    peers, x_hbm, gain_hbm, wk_hbm, wv_hbm, query_hbm, offset_hbm, out_gain_hbm,
    key_out, value_out, read_out,
    x, gain, wk, wv, query, offset, out_gain, kv, outbox, inbox,
    x_sem, in_sem, send_sem, recv_sem, own_sem, small_send, small_recv,
):
    rows = x.shape[0]
    width = wk.shape[1]
    spans = row_chunks(rows)
    chunks = len(spans)
    depth = width // peers
    me = lax.axis_index("sp")
    f32, bf16 = jnp.float32, jnp.bfloat16

    barrier = pltpu.get_barrier_semaphore()
    others = [lax.rem(me + d, peers) for d in range(1, peers)]
    for peer in others:
        pl.semaphore_signal(barrier, inc=1, device_id={"sp": peer}, device_id_type=MESH)

    def part(c):
        return pl.ds(*spans[c])

    loads = [
        pltpu.make_async_copy(src, dst, in_sem.at[i])
        for i, (src, dst) in enumerate(
            ((gain_hbm, gain), (wk_hbm, wk), (wv_hbm, wv), (query_hbm, query), (offset_hbm, offset), (out_gain_hbm, out_gain))
        )
    ]
    x_loads = [pltpu.make_async_copy(x_hbm.at[part(c), :], x.at[part(c), :], x_sem.at[c]) for c in range(chunks)]
    for copy in (loads[1], x_loads[0], loads[0], loads[2]):
        copy.start()

    outs = (key_out, value_out)
    left_half = 1 - (2 * me) // peers
    targets = []
    for j in range(peers - 1):
        down, up = peers - 1 - j, j
        down = down - (1 - (down - me + peers - 1) // peers)
        up = up + (1 - (me - up + peers - 1) // peers)
        targets.append(left_half * down + (1 - left_half) * up)

    def head_rows(place):
        return pl.ds(pl.multiple_of(place * depth, depth), depth)

    def send(kind, c, j):
        return pltpu.make_async_remote_copy(
            src_ref=kv.at[kind, head_rows(targets[j]), part(c)],
            dst_ref=outs[kind].at[me, :, part(c)],
            send_sem=send_sem.at[kind, c, j],
            recv_sem=recv_sem.at[kind, c, me],
            device_id={"sp": targets[j]},
            device_id_type=MESH,
        )

    def arrival(kind, c, j):
        return pltpu.make_async_remote_copy(
            src_ref=kv.at[kind, head_rows(targets[j]), part(c)],
            dst_ref=outs[kind].at[targets[j], :, part(c)],
            send_sem=send_sem.at[kind, c, j],
            recv_sem=recv_sem.at[kind, c, targets[j]],
            device_id={"sp": targets[j]},
            device_id_type=MESH,
        )

    def keep(kind, c):
        return pltpu.make_async_copy(
            kv.at[kind, head_rows(me), part(c)], outs[kind].at[me, :, part(c)], own_sem.at[kind, c]
        )

    def send_all(c, kinds, pieces):
        turn = 0 if c < chunks - 1 else peers // 2
        for j in [(turn + i) % (peers - 1) for i in pieces]:
            for kind in kinds:
                send(kind, c, j).start()

    loads[0].wait()
    gain_row = gain[...].reshape(1, -1)
    for c in range(chunks):
        x_loads[c].wait()
        if c == 0:
            for copy in x_loads[1:] + loads[3:]:
                copy.start()
        x32 = x[part(c), :].astype(f32)
        mean_square = jnp.mean(x32 * x32, axis=-1, keepdims=True)
        normed = (x32 * lax.rsqrt(mean_square + EPSILON) * gain_row).astype(bf16)
        for kind, weight in ((0, wk), (1, wv)):
            if c == 0:
                loads[1 + kind].wait()
            product = jnp.dot(normed, weight[...], preferred_element_type=f32)
            kv[kind, :, part(c)] = product.T.astype(bf16)
            if c == 0 and kind == 0:
                pl.semaphore_wait(barrier, peers - 1)
            send_all(c, (kind,), range(peers - 1 if c < chunks - 1 else peers - 2))
            keep(kind, c).start()

    for copy in loads[3:]:
        copy.wait()
    head_of = lax.broadcasted_iota(jnp.int32, (ROW_SLOTS, width), 1) // depth
    mine = head_of == lax.broadcasted_iota(jnp.int32, (ROW_SLOTS, width), 0)
    query_rows = jnp.where(mine, query[...].astype(f32).reshape(1, -1), 0.0).astype(bf16)
    slot = lax.broadcasted_iota(jnp.int32, (ROW_SLOTS, 1), 0)
    shift = jnp.zeros((ROW_SLOTS, 1), f32)
    for h in range(peers):
        shift = jnp.where(slot == h, offset[h], shift)
    scores = jnp.dot(query_rows, kv[0], preferred_element_type=f32) * depth ** (-0.5) + shift
    tiles = [scores[:, t * LANES:(t + 1) * LANES] for t in range(rows // LANES)]
    stacked = jnp.concatenate(tiles, axis=0)
    tail = jnp.log1p(jnp.exp(-jnp.abs(stacked)))
    remain = -jnp.maximum(stacked, 0.0) - tail
    later = lax.broadcasted_iota(jnp.int32, (LANES, LANES), 0) > lax.broadcasted_iota(jnp.int32, (LANES, LANES), 1)
    within = jnp.dot(remain, later.astype(f32), precision=lax.Precision.HIGHEST, preferred_element_type=f32)
    sums = jnp.sum(remain, axis=1, keepdims=True)
    running = jnp.zeros((ROW_SLOTS, 1), f32)
    beyond = [None] * len(tiles)
    for t in reversed(range(len(tiles))):
        beyond[t] = running
        running = running + sums[t * ROW_SLOTS:(t + 1) * ROW_SLOTS]
    sticks = jnp.exp(jnp.minimum(stacked, 0.0) - tail + within + jnp.concatenate(beyond, axis=0)).astype(bf16)
    sticks = jnp.concatenate([sticks[t * ROW_SLOTS:(t + 1) * ROW_SLOTS] for t in range(len(tiles))], axis=1)
    partial = lax.dot_general(sticks, kv[1], (((1,), (1,)), ((), ())), preferred_element_type=f32)
    zeros = jnp.zeros((ROW_SLOTS, width), f32)
    outbox[0:1, :] = jnp.sum(jnp.where(mine, partial, zeros), axis=0, keepdims=True)
    outbox[1:2, :] = jnp.sum(jnp.where(mine, running, zeros), axis=0, keepdims=True)

    def post(d):
        return pltpu.make_async_remote_copy(
            src_ref=outbox,
            dst_ref=inbox.at[d],
            send_sem=small_send.at[d - 1],
            recv_sem=small_recv.at[d - 1],
            device_id={"sp": lax.rem(me + d, peers)},
            device_id_type=MESH,
        )

    for d in range(1, peers):
        post(d).start()
    send_all(chunks - 1, (0, 1), (peers - 2,))

    for d in range(1, peers):
        post(d).wait_recv()
    totals, values = [outbox[1:2, :]], [outbox[0:1, :]]
    for d in range(1, peers):
        totals.append(inbox[d, 1:2, :])
        values.append(inbox[d, 0:1, :])
    places = [lax.rem(me - d + peers, peers) for d in range(peers)]
    mixed = jnp.zeros((1, width), f32)
    for d in range(peers):
        after = jnp.zeros((1, width), f32)
        for e in range(peers):
            if e != d:
                after = after + jnp.where(places[e] > places[d], totals[e], 0.0)
        mixed = mixed + values[d] * jnp.exp(after)
    spread = jnp.sum(jnp.where(mine, mixed * mixed, zeros), axis=1, keepdims=True) * (1.0 / depth)
    scale = jnp.sum(jnp.where(mine, lax.rsqrt(spread + EPSILON), zeros), axis=0, keepdims=True)
    read_out[...] = (mixed * scale * out_gain[...].reshape(1, -1)).astype(bf16).reshape(read_out.shape)

    for d in range(1, peers):
        post(d).wait_send()
    for c in range(chunks):
        for kind in range(2):
            keep(kind, c).wait()
            for j in range(peers - 1):
                send(kind, c, j).wait_send()
                arrival(kind, c, j).wait_recv()


def write_kernel(sources, targets, sems):
    copies = [pltpu.make_async_copy(src, dst, sems.at[i]) for i, (src, dst) in enumerate(zip(sources, targets))]
    for copy in copies:
        copy.start()
    for copy in copies:
        copy.wait()


def write_out(*arrays):
    count = len(arrays)

    def kernel(*refs):
        write_kernel(refs[:count], refs[count:2 * count], refs[2 * count])

    return pl.pallas_call(
        kernel,
        out_shape=tuple(jax.ShapeDtypeStruct(a.shape, a.dtype) for a in arrays),
        in_specs=[pl.BlockSpec(memory_space=pltpu.VMEM)] * count,
        out_specs=(pl.BlockSpec(memory_space=pltpu.HBM),) * count,
        scratch_shapes=[pltpu.SemaphoreType.DMA((count,))],
        compiler_params=pltpu.CompilerParams(vmem_limit_bytes=1024 * 1024),
        name="write_out",
    )(*arrays)


def fused_body(*arguments):
    prompt_rows, norm_gain, key_weight, value_weight, new_query, score_offset, output_gain = arguments
    peers = lax.axis_size("sp")
    rows, features = prompt_rows.shape
    width = key_weight.shape[1]
    depth = width // peers
    chunks = len(row_chunks(rows))
    f32, bf16 = jnp.float32, jnp.bfloat16
    vmem = pl.BlockSpec(memory_space=pltpu.VMEM)

    dma = pltpu.SemaphoreType.DMA
    cache = jax.ShapeDtypeStruct((peers, depth, rows), bf16)
    keys, values, read = pl.pallas_call(
        functools.partial(fused_kernel, peers),
        out_shape=(cache, cache, jax.ShapeDtypeStruct((width,), bf16)),
        in_specs=[pl.BlockSpec(memory_space=pltpu.HBM)] * 7,
        out_specs=(vmem, vmem, vmem),
        scratch_shapes=[
            pltpu.VMEM((rows, features), bf16),
            pltpu.VMEM((features,), f32),
            pltpu.VMEM((features, width), bf16),
            pltpu.VMEM((features, width), bf16),
            pltpu.VMEM((width,), bf16),
            pltpu.SMEM(score_offset.shape, f32),
            pltpu.VMEM((width,), f32),
            pltpu.VMEM((2, width, rows), bf16),
            pltpu.VMEM((2, width), f32),
            pltpu.VMEM((peers, 2, width), f32),
            dma((chunks,)),
            dma((6,)),
            dma((2, chunks, peers - 1)),
            dma((2, chunks, peers)),
            dma((2, chunks)),
            dma((peers - 1,)),
            dma((peers - 1,)),
        ],
        compiler_params=pltpu.CompilerParams(
            collective_id=0, has_side_effects=True, vmem_limit_bytes=VMEM_LIMIT
        ),
        name="fused_cache_read",
    )(*[pltpu.with_memory_space_constraint(argument, pltpu.HBM) for argument in arguments])

    keys, values, read = write_out(keys, values, read)

    def arrange(cache):
        return jnp.swapaxes(cache, 1, 2).reshape(1, 1, peers, rows, depth)

    return (arrange(keys), arrange(values), read)


def plain_body(prompt_rows, norm_gain, key_weight, value_weight, new_query, score_offset, output_gain):
    head_count = score_offset.shape[0]
    keys_here, values_here = project_rows(prompt_rows, norm_gain, key_weight, value_weight)
    keys_all, values_all = cache_layout(keys_here, values_here, head_count)
    local_keys, local_values = project_rows(prompt_rows, norm_gain, key_weight, value_weight)
    mixed = read_early(new_query, local_keys, local_values, score_offset)
    return (keys_all, values_all, finish_read(mixed, output_gain, head_count))


def body(prompt_rows, norm_gain, key_weight, value_weight, new_query, score_offset, output_gain):
    arguments = (prompt_rows, norm_gain, key_weight, value_weight, new_query, score_offset, output_gain)
    heads, devices = score_offset.shape[0], lax.axis_size("sp")
    rows, depth = prompt_rows.shape[0], key_weight.shape[1] // heads
    if heads == devices and heads <= 8 and rows % LANES == 0 and depth % 16 == 0 and key_weight.shape[1] % LANES == 0:
        return fused_body(*arguments)
    return plain_body(*arguments)


def solution(mesh):
    in_specs = (
        P(("grp", "sp"), None),
        P(),
        P(None, "tp"),
        P(None, "tp"),
        P(("grp", "tp")),
        P("tp"),
        P("tp"),
    )
    out_specs = (
        P(("grp", "tp"), "sp", None, None, None),
        P(("grp", "tp"), "sp", None, None, None),
        P(("grp", "tp")),
    )
    return jax.shard_map(body, mesh=mesh, in_specs=in_specs, out_specs=out_specs, check_vma=False)
```
